512 devices in a mesh: sp: 64 (over z, y), tp: 8 (over x, core).
Axes of the slice: x: 4, y: 4, z: 16, core: 2. Of those that a mesh axis runs over, the one named last changes fastest.
Arguments:
- prompt: bfloat16 [2, 12288, 4096], P(None, 'sp'), as said below
- w_key: bfloat16 [4096, 2048], P('sp', 'tp'), may hold values from -0.09375 to 0.09375
- w_value: bfloat16 [4096, 4096], P('sp', 'tp'), may hold values from -0.09375 to 0.09375
- w_igate: bfloat16 [4096, 8], replicated, may hold values from -0.09375 to 0.09375
- w_fgate: bfloat16 [4096, 8], replicated, may hold values from -0.09375 to 0.09375
- input_bias: float32 [8], replicated, may hold values from -1 to 120
- forget_bias: float32 [8], replicated, may hold values from 4 to 20
- new_query: bfloat16 [2, 8, 256], P(None, 'tp'), may hold values from -6 to 6
- new_key: bfloat16 [2, 8, 256], P(None, 'tp'), may hold values from -6 to 6
- new_value: bfloat16 [2, 8, 512], P(None, 'tp'), may hold values from -6 to 6
- new_gates: float32 [2, 2, 8], P(None, None, 'tp'), may hold values from 2 to 9
Outputs:
- cache_memory: bfloat16 [2, 8, 256, 512], P(None, 'tp', 'sp')
- cache_norm: float32 [2, 8, 256], P(None, 'tp', 'sp')
- cache_max: float32 [2, 8], P(None, 'tp')
- first_read: bfloat16 [2, 8, 512], P(None, 'tp')
The draws below stay inside these ranges and needn't reach their ends.
Inputs may be any that keep to these rules, and one draw needn't show every extreme that they name: `prompt`: Real-valued features, each entry drawn independently; their magnitude differs from one block of 192 positions to the next.
All inputs are finite; a program needn't handle non-finite values.
Results may differ from the reference program's by a relative error of at most 0.019.
Values may be sent and summed in bfloat16 or wider, within the bound.
A program may use at most 64 MiB of HBM per device.

```python
import math
import jax
import jax.numpy as jnp
from jax import lax

D = 4096
HEADS = 8
DK = 256
DV = 512
SEQS = 2
SPAN = 192
LEN = 12288


def draw_prompt(key, part):
    first, second = jax.random.split(jax.random.fold_in(key, 11))
    base = jax.random.normal(first, (SEQS, LEN // SPAN, SPAN, D), jnp.float32)
    lower, upper = (0.6, 1.7)
    scales = jnp.exp(jax.random.uniform(second, (SEQS, LEN // SPAN, 1, 1), jnp.float32, math.log(lower), math.log(upper)))
    return (base * scales).reshape(SEQS, LEN, D).astype(jnp.bfloat16)


def draw_input_bias(key, part):
    inner = jax.random.fold_in(key, 23)
    return jax.random.uniform(inner, (HEADS,), jnp.float32, -1.0, 1.0)


def draw_forget_bias(key, part):
    first, second, third = jax.random.split(jax.random.fold_in(key, 37), 3)
    picks = jax.random.randint(first, (HEADS,), 0, 8)
    quick = picks < 4
    slow_value = math.log(float(LEN)) + jax.random.uniform(second, (HEADS,), jnp.float32, 1.5, 2.5)
    quick_value = jax.random.uniform(third, (HEADS,), jnp.float32, 4.0, 5.0)
    return jnp.where(quick, quick_value, slow_value)


def shard_levels(own_key, dims, cuts, least, top_value):
    level = 1.0
    for position, parts in cuts:
        heights = jax.random.uniform(jax.random.fold_in(jax.random.fold_in(own_key, 6), position), (parts,), jnp.float32, least / len(cuts), top_value / len(cuts))
        level = level * jnp.repeat(jnp.exp(heights), dims[position] // parts).reshape((-1,) + (1,) * (len(dims) - 1 - position))
    return level


def normal_values(own_key, dims, deviation, limit, shards=(), held_as=jnp.bfloat16):
    result = deviation * jax.random.normal(own_key, dims, jnp.float32)
    if shards:
        result = result * shard_levels(own_key, dims, shards, -0.22, 0.18)
    return jnp.clip(result, -limit, limit).astype(held_as)


def setup_inputs(seed: int = 0) -> dict:
    key_list = jax.random.split(jax.random.key(seed), 12)
    prompt = draw_prompt(jax.random.fold_in(key_list[11], 71), 0)
    w_key = normal_values(key_list[1], (D, HEADS * DK), D ** -0.5, 0.09375, ((0, 64), (1, 8)))
    w_value = normal_values(key_list[2], (D, HEADS * DV), D ** -0.5, 0.09375, ((0, 64), (1, 8)))
    w_igate = normal_values(key_list[3], (D, HEADS), D ** -0.5, 0.09375)
    w_fgate = normal_values(key_list[4], (D, HEADS), D ** -0.5, 0.09375)
    input_bias = draw_input_bias(jax.random.fold_in(key_list[11], 71), 0)
    forget_bias = draw_forget_bias(jax.random.fold_in(key_list[11], 71), 0)
    new_query = normal_values(key_list[7], (SEQS, HEADS, DK), 1.0, 6.0, ((1, 8),))
    new_key = normal_values(key_list[8], (SEQS, HEADS, DK), 1.0, 6.0, ((1, 8),))
    new_value = normal_values(key_list[9], (SEQS, HEADS, DV), 1.0, 6.0, ((1, 8),))
    new_gates = jnp.clip(2.0 + 7.0 * jax.random.uniform(key_list[10], (2, SEQS, HEADS), jnp.float32) ** shard_levels(key_list[10], (2, SEQS, HEADS), ((2, 8),), -0.2, 0.2), 2.0, 9.0)
    return {"prompt": prompt, "w_key": w_key, "w_value": w_value, "w_igate": w_igate, "w_fgate": w_fgate, "input_bias": input_bias, "forget_bias": forget_bias, "new_query": new_query, "new_key": new_key, "new_value": new_value, "new_gates": new_gates}


def reference(prompt, w_key, w_value, w_igate, w_fgate, input_bias, forget_bias, new_query, new_key, new_value, new_gates):
    blocks = LEN // SPAN
    token_rows = prompt.reshape(SEQS * LEN, D)
    key_rows = jnp.dot(token_rows, w_key, preferred_element_type=jnp.float32).astype(jnp.bfloat16)
    value_rows = jnp.dot(token_rows, w_value, preferred_element_type=jnp.float32).astype(jnp.bfloat16)
    input_gate = jnp.dot(token_rows, w_igate, preferred_element_type=jnp.float32) + input_bias
    log_forget = jax.nn.log_sigmoid(jnp.dot(token_rows, w_fgate, preferred_element_type=jnp.float32) + forget_bias)
    input_gate = input_gate.reshape(SEQS, blocks, SPAN, HEADS)
    log_forget = log_forget.reshape(SEQS, blocks, SPAN, HEADS)
    block_total = jnp.sum(log_forget, axis=2)
    forget_after = block_total[:, :, None] - jnp.cumsum(log_forget, axis=2)
    log_weight = forget_after + input_gate
    block_max = jnp.max(log_weight, axis=2)
    later_total = jnp.flip(jnp.cumsum(jnp.flip(block_total, 1), axis=1), 1) - block_total
    block_lift = later_total + block_max
    global_max = jnp.max(block_lift, axis=1)
    factor = jnp.exp(block_lift - global_max[:, None])
    key_scale = DK ** -0.5
    key_blocks = key_rows.reshape(SEQS, blocks, SPAN, HEADS, DK).astype(jnp.float32)
    decayed = (jnp.exp(log_weight - block_max[:, :, None])[..., None] * key_scale * key_blocks).astype(jnp.bfloat16)
    value_blocks = value_rows.reshape(SEQS, blocks, SPAN, HEADS, DV)

    def accumulate(carry, inputs):
        memory, normal = carry
        block_keys, block_values, block_factor = inputs
        block_state = jnp.einsum('sthk,sthv->shkv', block_keys.astype(jnp.float32), block_values.astype(jnp.float32),
                                 precision=lax.Precision.HIGHEST)
        block_norm = jnp.sum(block_keys.astype(jnp.float32), axis=1)
        memory = memory + block_factor[:, :, None, None] * block_state
        normal = normal + block_factor[:, :, None] * block_norm
        return (memory, normal), None

    inputs = (jnp.moveaxis(decayed, 1, 0), jnp.moveaxis(value_blocks, 1, 0), jnp.moveaxis(factor, 1, 0))
    start = (jnp.zeros((SEQS, HEADS, DK, DV), jnp.float32), jnp.zeros((SEQS, HEADS, DK), jnp.float32))
    (memory, normal), _ = lax.scan(accumulate, start, inputs)
    query_full = new_query.astype(jnp.float32)
    query_state = jnp.einsum('shk,shkv->shv', query_full, memory, precision=lax.Precision.HIGHEST)
    query_norm = jnp.sum(query_full * normal, axis=-1)
    forget_new = jax.nn.log_sigmoid(new_gates[1])
    input_new = new_gates[0]
    mixed = jnp.maximum(forget_new + global_max, input_new)
    carried = jnp.exp(forget_new + global_max - mixed)
    fresh = jnp.exp(input_new - mixed)
    own_score = jnp.sum(query_full * new_key.astype(jnp.float32), axis=-1) * key_scale
    numer = carried[..., None] * query_state + (fresh * own_score)[..., None] * new_value.astype(jnp.float32)
    denom = carried * query_norm + fresh * own_score
    first_read = (numer / jnp.maximum(jnp.abs(denom), 1.0)[..., None]).astype(jnp.bfloat16)
    return memory.astype(jnp.bfloat16), normal, global_max, first_read
```

```python
import jax
import jax.numpy as jnp
from jax import lax
from jax.experimental import pallas as pl
from jax.experimental.pallas import tpu as pltpu
from jax.sharding import PartitionSpec as P

F32 = jnp.float32
BF16 = jnp.bfloat16
Y = 4
KR = 256


def log_sigmoid(x):
    e = jnp.exp(-jnp.abs(x))
    series = e * (1.0 - e * (0.5 - e * (1.0 / 3.0 - e * (0.25 - e * 0.2))))
    return jnp.minimum(x, 0.0) - jnp.where(e < 0.04, series, jnp.log(1.0 + e))


def three(x):
    hi = x.astype(BF16).astype(F32)
    mid = (x - hi).astype(BF16).astype(F32)
    return hi, mid, x - hi - mid


def kernel(
    nz, nx,
    prompt, wk, wv, wi, wf, ib, fb, nq, nk, nv, ng,
    o_mem, o_norm, o_max, o_read,
    XB, WI, WF, WK, WV, AK, AV, GM, ST, PB, KC, VE, SC, SF, SB, R1, S2, R2, QM, QR, MB, RB,
    s_loc, s_ag, r_ag, s_yk, r_yk, s_sw, r_sw, s_tx, r_tx, s_st, r_st, s_qm, r_qm, s_ys, r_ys, s_zs, r_zs,
):
    sp = lax.axis_index("sp")
    tp = lax.axis_index("tp")
    z, y = sp // Y, sp % Y
    x, c = tp // 2, tp % 2
    parity = y // 2
    swapped = c != parity
    native = c == parity
    role = jnp.where(swapped, 1, 0)
    yr = jnp.where(swapped, 3 - y, y)
    yo = yr + 1 - 2 * (yr % 2)
    y1 = y + 1 - 2 * (y % 2)
    scale = 256 ** -0.5

    def at(x_, y_, z_, c_):
        return (z_ * Y + y_, x_ * 2 + c_)

    def wrap(v, n):
        return (v + n) % n

    zp, zm = at(x, y, wrap(z + 1, nz), c), at(x, y, wrap(z - 1, nz), c)
    xp, xm = at(wrap(x + 1, nx), y, z, c), at(wrap(x - 1, nx), y, z, c)
    sib, yp, diag = at(x, y, z, 1 - c), at(x, y1, z, c), at(x, y1, z, 1 - c)
    partner = at(x, 3 - y, z, 1 - c)

    def rc(src, dst, ss, rs, dev):
        return pltpu.make_async_remote_copy(
            src_ref=src, dst_ref=dst, send_sem=ss, recv_sem=rs, device_id=dev,
            device_id_type=pl.DeviceIdType.MESH)

    def rows(ref, start, n):
        return ref.at[pl.ds(pl.multiple_of(start, 32), n)]

    l_prompt = pltpu.make_async_copy(prompt, XB.at[0], s_loc.at[0])
    l_wi = pltpu.make_async_copy(wi, WI, s_loc.at[1])
    l_wf = pltpu.make_async_copy(wf, WF, s_loc.at[2])
    own_k = rows(WK, z * KR + yr * 64, 64)
    own_v = rows(WV, z * KR + yr * 64, 64)
    l_wk = pltpu.make_async_copy(wk, own_k, s_loc.at[3])
    l_wv = pltpu.make_async_copy(wv, own_v, s_loc.at[4])

    @pl.when(native)
    def _():
        l_wv.start()
        l_wk.start()

    l_prompt.start()
    l_wi.start()
    l_wf.start()

    barrier = pltpu.get_barrier_semaphore()
    for dev in (zp, zm, xp, xm, sib, yp, diag, partner):
        pl.semaphore_signal(barrier, inc=1, device_id=dev, device_id_type=pl.DeviceIdType.MESH)
    pl.semaphore_wait(barrier, 8)

    sw_v = rc(wv, rows(WV, z * KR + y * 64, 64), s_sw.at[0], r_sw.at[0], partner)
    sw_k = rc(wk, rows(WK, z * KR + y * 64, 64), s_sw.at[1], r_sw.at[1], partner)
    sw_g = rc(GM.at[0], GM.at[1], s_sw.at[2], r_sw.at[2], partner)

    def tok(xx, j, half=None):
        cols = pl.ds(pl.multiple_of((xx * 4 + j) * 256, 256), 256)
        if half is None:
            return XB.at[1, :, :, cols]
        return XB.at[1, half, :, cols]

    def sw_t(j):
        cols = pl.ds(pl.multiple_of((x * 4 + j) * 256, 256), 256)
        return rc(prompt.at[:, :, cols], tok(x, j), s_sw.at[3 + j], r_sw.at[3 + j], partner)

    def t1(way, j, xx):
        return rc(tok(xx, j), tok(xx, j), s_tx.at[way, j], r_tx.at[way, j], (xp, xm)[way])

    def t2(way, j, xx):
        q = wrap(xx - 1, nx) if way == 0 else wrap(xx + 1, nx)
        return rc(tok(q, j, way), tok(q, j, way), s_tx.at[2 + way, j], r_tx.at[2 + way, j], (xp, xm)[way])

    @pl.when(swapped)
    def _():
        sw_v.start()
        sw_k.start()
        for j in range(4):
            sw_t(j).start()

    def zk(way, s, zz):
        b = wrap(zz - (s - 1), nz) if way == 0 else wrap(zz + (s - 1), nz)
        ref = rows(WK, b * KR + c * 128, 128) if s < 8 else rows(WK, b * KR + c * 128 + way * 64, 64)
        return rc(ref, ref, s_ag.at[way, s], r_ag.at[way, s], (zp, zm)[way])

    def zv(way, s, zz, who):
        b = wrap(zz - (s - 1), nz) if way == 0 else wrap(zz + (s - 1), nz)
        ref = rows(WV, b * KR + who * 64, 64) if s < 8 else rows(WV, b * KR + who * 64 + way * 32, 32)
        return rc(ref, ref, s_ag.at[2 + way, s], r_ag.at[2 + way, s], (zp, zm)[way])

    def blocks(s):
        if s == 0 or s == 8:
            return ((0, wrap(z - s, nz)),)
        return ((0, wrap(z - s, nz)), (1, wrap(z + s, nz)))

    def yv(s, who):
        out = []
        for k, b in blocks(s):
            ref = rows(WV, b * KR + who * 64, 64)
            out.append(rc(ref, ref, s_ag.at[4 + k, s], r_ag.at[4 + k, s], yp))
        return out

    def dk(s, cc):
        out = []
        for k, b in blocks(s):
            ref = rows(WK, b * KR + cc * 128, 128)
            out.append(rc(ref, ref, s_ag.at[6 + k, s], r_ag.at[6 + k, s], sib))
        return out

    def dv(s, cc):
        out = []
        for k, b in blocks(s):
            ref = rows(WV, b * KR + cc * 128, 128)
            out.append(rc(ref, ref, s_ag.at[8 + k, s], r_ag.at[8 + k, s], sib))
        return out

    def start(copies):
        for cp in copies:
            cp.start()

    def wait_recv(copies):
        for cp in copies:
            cp.wait_recv()

    yk_send = rc(own_k, own_k, s_yk.at[0], r_yk.at[0], yp)
    other_k = rows(WK, z * KR + yo * 64, 64)
    yk_recv = rc(other_k, other_k, s_yk.at[0], r_yk.at[0], yp)
    got_v = rc(own_v, own_v, s_sw.at[0], r_sw.at[0], partner)
    got_k = rc(own_k, own_k, s_sw.at[1], r_sw.at[1], partner)

    @pl.when(native)
    def _():
        l_wv.wait()

    @pl.when(swapped)
    def _():
        got_v.wait_recv()

    zv(0, 1, z, yr).start()
    zv(1, 1, z, yr).start()

    @pl.when(native)
    def _():
        l_wk.wait()

    @pl.when(swapped)
    def _():
        got_k.wait_recv()

    yk_send.start()
    start(yv(0, yr))
    yk_recv.wait_recv()
    zk(0, 1, z).start()
    zk(1, 1, z).start()
    start(dk(0, c))

    l_prompt.wait()
    l_wi.wait()
    l_wf.wait()
    tokens = XB[0].reshape(384, 4096)
    lane8 = lax.broadcasted_iota(jnp.int32, (384, 8), 1)

    def gate(w, b):
        g = jnp.dot(tokens, w[...], preferred_element_type=F32)
        g = jnp.sum(jnp.where(lane8 == tp, g, 0.0), axis=1, keepdims=True) + b
        return jnp.broadcast_to(g, (384, 128))

    gi = gate(WI, ib[tp])
    lf = log_sigmoid(gate(WF, fb[tp]))
    after = (lax.broadcasted_iota(jnp.int32, (192, 192), 1)
             > lax.broadcasted_iota(jnp.int32, (192, 192), 0)).astype(F32)
    row8 = lax.broadcasted_iota(jnp.int32, (8, 128), 0)
    stats = jnp.zeros((8, 128), F32)
    qtile = jnp.zeros((8, 128), F32)
    for s in range(2):
        part = lf[s * 192:(s + 1) * 192]
        lw = jnp.dot(after, part, precision=lax.Precision.HIGHEST, preferred_element_type=F32)
        lw = lw + gi[s * 192:(s + 1) * 192]
        total = jnp.sum(part, axis=0, keepdims=True)
        top = jnp.max(lw, axis=0, keepdims=True)
        GM[0, s * 192:(s + 1) * 192, :] = jnp.exp(lw - top) * scale
        stats = jnp.where(row8 == 2 * s, total, jnp.where(row8 == 2 * s + 1, top, stats))
        qs = nq[s].astype(F32)
        qtile = jnp.where(row8 == 2 * s, qs[:, :128], jnp.where(row8 == 2 * s + 1, qs[:, 128:], qtile))
    GM[0, 384:392, :] = stats
    GM[0, 392:400, :] = qtile

    @pl.when(swapped)
    def _():
        sw_g.start()

    AK[...] = jnp.zeros_like(AK)
    AV[...] = jnp.zeros_like(AV)
    VE[:, 512:640] = jnp.ones((384, 128), BF16)
    kk = lax.broadcasted_iota(jnp.int32, (256, 512), 0)
    rr = lax.broadcasted_iota(jnp.int32, (256, 512), 1)
    for s in range(2):
        target = ((kk >> 2) & 3) * 128 + (kk >> 4) * 8 + s * 4 + (kk & 3)
        PB[s] = (rr == target).astype(F32).astype(BF16)

    def st(k):
        return rc(GM.at[role, pl.ds(384, 8)], ST.at[yr], s_st.at[k], r_st.at[k], (sib, yp, diag)[k])

    def step(s):
        zk(0, s, z - 1).wait_recv()
        if s < 8:
            zk(0, s + 1, z).start()
        zk(1, s, z + 1).wait_recv()
        if s < 8:
            zk(1, s + 1, z).start()
        start(dk(s, c))
        zv(0, s, z - 1, yr).wait_recv()
        if s < 8:
            zv(0, s + 1, z, yr).start()
        zv(1, s, z + 1, yr).wait_recv()
        if s < 8:
            zv(1, s + 1, z, yr).start()
        start(yv(s, yr))
        wait_recv(yv(s - 1, yo))
        start(dv(s - 1, c))

    def token_step(s):
        if s <= 5:
            @pl.when(swapped)
            def _():
                if s <= 4:
                    j = s - 1
                    got = rc(tok(x, j), tok(x, j), s_sw.at[3 + j], r_sw.at[3 + j], partner)
                    got.wait_recv()
                    t1(0, j, x).start()
                    t1(1, j, x).start()
                if s >= 2:
                    j = s - 2
                    t1(0, j, wrap(x - 1, nx)).wait_recv()
                    t2(0, j, x).start()
                    t1(1, j, wrap(x + 1, nx)).wait_recv()
                    t2(1, j, x).start()

    for s in range(1, 4):
        step(s)
        token_step(s)

    @pl.when(swapped)
    def _():
        sw_g.wait_recv()

    ST[yr] = GM[role, 384:392, :]
    for k in range(3):
        st(k).start()
    step(4)
    token_step(4)
    step(5)
    token_step(5)
    for k in range(3):
        st(k).wait_recv()
    mz, tz = [], []
    for s in range(2):
        later = jnp.zeros((1, 128), F32)
        lifts = [None] * Y
        for k in reversed(range(Y)):
            lifts[k] = ST[k, 2 * s + 1:2 * s + 2, :] + later
            later = later + ST[k, 2 * s:2 * s + 1, :]
        top = jnp.maximum(jnp.maximum(lifts[0], lifts[1]), jnp.maximum(lifts[2], lifts[3]))
        mine = lifts[3]
        for k in range(3):
            mine = jnp.where(yr == k, lifts[k], mine)
        SC[s * 192:(s + 1) * 192, :] = GM[role, s * 192:(s + 1) * 192, :] * jnp.exp(mine - top)
        mz.append(top)
        tz.append(later)
    step(6)
    step(7)

    @pl.when(swapped)
    def _():
        for j in range(4):
            t2(0, j, wrap(x - 1, nx)).wait_recv()
            t2(1, j, wrap(x + 1, nx)).wait_recv()

    def mm(b):
        xc = XB[role, :, :, pl.ds(pl.multiple_of(b * KR, KR), KR)].reshape(384, KR)
        r = pl.ds(pl.multiple_of(b * KR, KR), KR)
        AK[...] += jnp.dot(xc, WK[r, :], preferred_element_type=F32)
        AV[...] += jnp.dot(xc, WV[r, :], preferred_element_type=F32)

    def wait_d(s):
        wait_recv(dk(s, 1 - c))
        wait_recv(dv(s, 1 - c))

    def mm_pair(s):
        def one(i, carry):
            mm(wrap(z + (2 * i - 1) * s, nz))
            return carry
        lax.fori_loop(0, 2, one, 0)

    for s in range(6):
        wait_d(s)

    def early(i, carry):
        mm(wrap(z + i - 5, nz))
        return carry

    lax.fori_loop(0, 11, early, 0)
    step(8)
    wait_d(6)
    mm_pair(6)
    wait_recv(yv(8, yo))
    start(dv(8, c))
    wait_d(7)
    mm_pair(7)
    wait_d(8)
    mm(wrap(z + 8, nz))

    for s in range(2):
        sc = SC[s * 192:(s + 1) * 192, :]
        kd = (AK[s * 192:(s + 1) * 192, :] * jnp.concatenate([sc, sc], axis=1)).astype(BF16)
        KC[s * 192:(s + 1) * 192, :] = jnp.dot(kd, PB[s], preferred_element_type=F32).astype(BF16)
    VE[:, 0:512] = AV[...].astype(BF16)

    def state(h):
        cols = pl.ds(pl.multiple_of(h * 256, 256), 256)
        out = lax.dot_general(KC[:, cols], VE[...], (((0,), (0,)), ((), ())), preferred_element_type=F32)
        SF[cols, :] = out
        SB[cols, :] = out.astype(BF16)

    ys1 = rc(rows(SB, (1 - c) * 256, 256), R1, s_ys.at[0], r_ys.at[0], sib)
    ys2 = rc(S2, R2, s_ys.at[1], r_ys.at[1], yp)
    state(1 - c)
    ys1.start()
    state(c)
    qsum = []
    sf_lo = (SF[...] - SB[...].astype(F32)).astype(BF16)
    for s in range(2):
        qs = jnp.concatenate([GM[role, 392 + 2 * s:393 + 2 * s, :], GM[role, 393 + 2 * s:394 + 2 * s, :]], axis=1)
        qs = jnp.broadcast_to(qs, (16, 256)).astype(BF16)
        qc = jnp.dot(qs, PB[s], preferred_element_type=F32).astype(BF16)
        full = jnp.dot(qc, SB[...], preferred_element_type=F32) + jnp.dot(qc, sf_lo, preferred_element_type=F32)
        qsum.append(full[0:8])
    row640 = lax.broadcasted_iota(jnp.int32, (8, 640), 0)
    both = jnp.where(row640 < 4, qsum[0], qsum[1])
    qt = jnp.zeros((8, 128), F32)
    for k in range(4):
        qt = qt + jnp.where((row8 & 3) == k, both[:, k * 128:(k + 1) * 128], 0.0)
    QM[0:8, :] = qt
    QM[8:16, :] = both[:, 512:640]

    def qm(k):
        return rc(QM, QR.at[k], s_qm.at[k], r_qm.at[k], (sib, yp, diag)[k])

    for k in range(3):
        qm(k).start()
    ys1.wait_recv()
    send_rows = pl.ds(pl.multiple_of(yo * 128, 128), 128)
    keep_rows = pl.ds(pl.multiple_of(yr * 128, 128), 128)
    send_part = pl.ds(pl.multiple_of((yo % 2) * 128, 128), 128)
    keep_part = pl.ds(pl.multiple_of((yr % 2) * 128, 128), 128)
    S2[...] = (SF[send_rows, :] + R1[send_part, :].astype(F32)).astype(BF16)
    ys2.start()
    kept = SF[keep_rows, :] + R1[keep_part, :].astype(F32)
    for k in range(3):
        qm(k).wait_recv()
    qall = QM[...] + QR[0] + QR[1] + QR[2]
    qt, qn = qall[0:8], qall[8:16]
    lane8 = lax.broadcasted_iota(jnp.int32, (8, 128), 1)
    head = jnp.zeros((8, 128), F32)
    m8 = jnp.where(row8 < 4, mz[0], mz[1])
    t8 = jnp.where(row8 < 4, tz[0], tz[1])
    for base, v in ((2, m8), (5, t8), (8, qn)):
        for i, piece in enumerate(three(v)):
            head = jnp.where(lane8 == base + i, piece, head)
    MB[:, :, 640:768] = jnp.broadcast_to(qt.astype(BF16)[None], (nz, 8, 128))
    ys2.wait_recv()
    kept = (kept + R2[...].astype(F32)).reshape(nz, 8, 640)
    MB[:, :, 0:512] = kept[:, :, 0:512].astype(BF16)
    norm = kept[:, :, 512:640]
    norm_hi = norm.astype(BF16).astype(F32)
    lane3 = lax.broadcasted_iota(jnp.int32, (nz, 8, 128), 2)
    tail = jnp.where(lane3 == 0, norm_hi, jnp.where(lane3 == 1, norm - norm_hi, head[None]))
    MB[:, :, 512:640] = tail.astype(BF16)

    oy = jnp.where(swapped, 3 - y, y)
    oc = jnp.where(swapped, 1 - c, c)

    def zs(to):
        return rc(MB.at[to], RB.at[z], s_zs.at[to], r_zs.at[z], at(x, oy, to, oc))

    def zs_recv(frm):
        return rc(MB.at[frm], RB.at[frm], s_zs.at[frm], r_zs.at[frm], at(x, oy, frm, oc))

    for d in (8, 7, -7, 6, -6, 5, -5, 4, -4, 3, -3, 2, -2, 1, -1):
        zs(wrap(z + d, nz)).start()

    @pl.when(swapped)
    def _():
        zs(z).start()

    @pl.when(native)
    def _():
        RB[z] = MB[z]

    for d in (1, -1, 2, -2, 3, -3, 4, -4, 5, -5, 6, -6, 7, -7, 8):
        zs_recv(wrap(z + d, nz)).wait_recv()

    @pl.when(swapped)
    def _():
        zs_recv(z).wait_recv()

    tails = RB[:, :, 512:640].astype(F32)
    m_all = jnp.sum(jnp.where((lane3 >= 2) & (lane3 < 5), tails, 0.0), axis=2, keepdims=True)
    t_all = jnp.sum(jnp.where((lane3 >= 5) & (lane3 < 8), tails, 0.0), axis=2, keepdims=True)
    later = jnp.zeros((8, 1), F32)
    lifts = [None] * nz
    for k in reversed(range(nz)):
        lifts[k] = m_all[k] + later
        later = later + t_all[k]
    top = lifts[0]
    for k in range(1, nz):
        top = jnp.maximum(top, lifts[k])
    acc = jnp.zeros((8, 768), F32)
    for k in range(nz):
        acc = acc + jnp.exp(lifts[k] - top) * RB[k].astype(F32)
    for s in range(2):
        o_mem[s, 0] = acc[4 * s:4 * s + 4, 0:512].astype(BF16)
        o_max[s] = top[4 * s]
    tail = acc[:, 512:640]
    norm = jnp.sum(jnp.where(lane8 < 2, tail, 0.0), axis=1, keepdims=True)
    qn = jnp.sum(jnp.where((lane8 >= 8) & (lane8 < 11), tail, 0.0), axis=1, keepdims=True)
    for s in range(2):
        line = jnp.sum(jnp.where(row8 - 4 * s == lane8, norm, 0.0), axis=0, keepdims=True)
        o_norm[s] = line[:, 0:4]
    row1 = lax.broadcasted_iota(jnp.int32, (8, 1), 0)
    gate_in = jnp.where(row1 < 4, ng[0, 0:1, :], ng[0, 1:2, :])
    gate_forget = log_sigmoid(jnp.where(row1 < 4, ng[1, 0:1, :], ng[1, 1:2, :]))
    own = [jnp.sum(nq[s].astype(F32) * nk[s].astype(F32), axis=1, keepdims=True) * scale for s in range(2)]
    own = jnp.where(row1 < 4, own[0], own[1])
    mixed = jnp.maximum(gate_forget + top, gate_in)
    carried = jnp.exp(gate_forget + top - mixed)
    fresh = jnp.exp(gate_in - mixed)
    value = jnp.zeros((8, 128), F32)
    for s in range(2):
        for k in range(4):
            value = jnp.where(row8 == 4 * s + k, nv[s].astype(F32)[:, k * 128:(k + 1) * 128], value)
    numer = carried * acc[:, 640:768] + fresh * own * value
    denom = carried * qn + fresh * own
    read = numer / jnp.maximum(jnp.abs(denom), 1.0)
    for s in range(2):
        for k in range(4):
            o_read[s, :, k * 128:(k + 1) * 128] = read[4 * s + k:4 * s + k + 1].astype(BF16)

    for s in range(1, 9):
        for way in range(2):
            zk(way, s, z).wait_send()
            zv(way, s, z, yr).wait_send()
    for s in range(9):
        for cp in yv(s, yr) + dk(s, c) + dv(s, c):
            cp.wait_send()
    yk_send.wait_send()
    for k in range(3):
        st(k).wait_send()
        qm(k).wait_send()
    ys1.wait_send()
    ys2.wait_send()
    for d in range(1, 16):
        zs(wrap(z + d - 16, nz)).wait_send()

    @pl.when(swapped)
    def _():
        zs(z).wait_send()
        sw_v.wait_send()
        sw_k.wait_send()
        sw_g.wait_send()
        for j in range(4):
            sw_t(j).wait_send()
            for way in range(2):
                t1(way, j, x).wait_send()
                t2(way, j, x).wait_send()


def per_device(*args):
    nz = lax.axis_size("sp") // Y
    nx = lax.axis_size("tp") // 2
    vm = pl.BlockSpec(memory_space=pltpu.VMEM)
    sm = pl.BlockSpec(memory_space=pltpu.SMEM)
    hb = pl.BlockSpec(memory_space=pltpu.HBM)
    dma = pltpu.SemaphoreType.DMA
    return pl.pallas_call(
        lambda *refs: kernel(nz, nx, *refs),
        out_shape=(
            jax.ShapeDtypeStruct((2, 1, 4, 512), BF16),
            jax.ShapeDtypeStruct((2, 1, 4), F32),
            jax.ShapeDtypeStruct((2, 1), F32),
            jax.ShapeDtypeStruct((2, 1, 512), BF16),
        ),
        in_specs=[hb] * 5 + [sm] * 2 + [vm] * 4,
        out_specs=(vm,) * 4,
        scratch_shapes=[
            pltpu.VMEM((2, 2, 192, 4096), BF16),
            pltpu.VMEM((4096, 8), BF16),
            pltpu.VMEM((4096, 8), BF16),
            pltpu.VMEM((4096, 256), BF16),
            pltpu.VMEM((4096, 512), BF16),
            pltpu.VMEM((384, 256), F32),
            pltpu.VMEM((384, 512), F32),
            pltpu.VMEM((2, 400, 128), F32),
            pltpu.VMEM((4, 8, 128), F32),
            pltpu.VMEM((2, 256, 512), BF16),
            pltpu.VMEM((384, 512), BF16),
            pltpu.VMEM((384, 640), BF16),
            pltpu.VMEM((384, 128), F32),
            pltpu.VMEM((512, 640), F32),
            pltpu.VMEM((512, 640), BF16),
            pltpu.VMEM((256, 640), BF16),
            pltpu.VMEM((128, 640), BF16),
            pltpu.VMEM((128, 640), BF16),
            pltpu.VMEM((16, 128), F32),
            pltpu.VMEM((3, 16, 128), F32),
            pltpu.VMEM((nz, 8, 768), BF16),
            pltpu.VMEM((nz, 8, 768), BF16),
            dma((5,)),
            dma((10, 9)), dma((10, 9)),
            dma((1,)), dma((1,)),
            dma((7,)), dma((7,)),
            dma((4, 4)), dma((4, 4)),
            dma((3,)), dma((3,)),
            dma((3,)), dma((3,)),
            dma((2,)), dma((2,)),
            dma((nz,)), dma((nz,)),
        ],
        compiler_params=pltpu.CompilerParams(
            collective_id=0, has_side_effects=True, vmem_limit_bytes=56 * 1024 * 1024),
        name="prefill",
    )(*args)


def solution(mesh):
    placed = (
        P(None, "sp", None),
        P("sp", "tp"),
        P("sp", "tp"),
        P(),
        P(),
        P(),
        P(),
        P(None, "tp", None),
        P(None, "tp", None),
        P(None, "tp", None),
        P(None, None, "tp"),
    )
    return jax.shard_map(
        per_device,
        mesh=mesh,
        in_specs=placed,
        out_specs=(
            P(None, "tp", "sp", None),
            P(None, "tp", "sp"),
            P(None, "tp"),
            P(None, "tp", None),
        ),
        check_vma=False,
    )
```

```python
import jax
import jax.numpy as jnp
from jax import lax
from jax.experimental import pallas as pl
from jax.experimental.pallas import tpu as pltpu
from jax.sharding import PartitionSpec as P

F32 = jnp.float32
BF16 = jnp.bfloat16
Y = 4
KR = 256


def log_sigmoid(x):
    e = jnp.exp(-jnp.abs(x))
    series = e * (1.0 - e * (0.5 - e * (1.0 / 3.0 - e * (0.25 - e * 0.2))))
    return jnp.minimum(x, 0.0) - jnp.where(e < 0.04, series, jnp.log(1.0 + e))


def three(x):
    hi = x.astype(BF16).astype(F32)
    mid = (x - hi).astype(BF16).astype(F32)
    return hi, mid, x - hi - mid


def kernel(
    nz, nx,
    prompt, wk, wv, wi, wf, ib, fb, nq, nk, nv, ng,
    out,
    XB, WI, WF, WK, WV, AK, AV, GM, ST, PB, KC, VE, SC, SF, SB, R1, S2, R2, QM, QR, MB, RB,
    s_loc, s_ag, r_ag, s_yk, r_yk, s_sw, r_sw, s_tx, r_tx, s_st, r_st, s_qm, r_qm, s_ys, r_ys, s_zs, r_zs,
):
    sp = lax.axis_index("sp")
    tp = lax.axis_index("tp")
    z, y = sp // Y, sp % Y
    x, c = tp // 2, tp % 2
    parity = y // 2
    swapped = c != parity
    native = c == parity
    role = jnp.where(swapped, 1, 0)
    yr = jnp.where(swapped, 3 - y, y)
    yo = yr + 1 - 2 * (yr % 2)
    y1 = y + 1 - 2 * (y % 2)
    scale = 256 ** -0.5

    def at(x_, y_, z_, c_):
        return (z_ * Y + y_, x_ * 2 + c_)

    def wrap(v, n):
        return (v + n) % n

    zp, zm = at(x, y, wrap(z + 1, nz), c), at(x, y, wrap(z - 1, nz), c)
    xp, xm = at(wrap(x + 1, nx), y, z, c), at(wrap(x - 1, nx), y, z, c)
    sib, yp, diag = at(x, y, z, 1 - c), at(x, y1, z, c), at(x, y1, z, 1 - c)
    partner = at(x, 3 - y, z, 1 - c)

    def rc(src, dst, ss, rs, dev):
        return pltpu.make_async_remote_copy(
            src_ref=src, dst_ref=dst, send_sem=ss, recv_sem=rs, device_id=dev,
            device_id_type=pl.DeviceIdType.MESH)

    def rows(ref, start, n):
        return ref.at[pl.ds(pl.multiple_of(start, 32), n)]

    l_prompt = pltpu.make_async_copy(prompt, XB.at[0], s_loc.at[0])
    l_wi = pltpu.make_async_copy(wi, WI, s_loc.at[1])
    l_wf = pltpu.make_async_copy(wf, WF, s_loc.at[2])
    own_k = rows(WK, z * KR + yr * 64, 64)
    own_v = rows(WV, z * KR + yr * 64, 64)
    l_wk = pltpu.make_async_copy(wk, own_k, s_loc.at[3])
    l_wv = pltpu.make_async_copy(wv, own_v, s_loc.at[4])

    @pl.when(native)
    def _():
        l_wv.start()
        l_wk.start()

    l_prompt.start()
    l_wi.start()
    l_wf.start()

    barrier = pltpu.get_barrier_semaphore()
    for dev in (zp, zm, xp, xm, sib, yp, diag, partner):
        pl.semaphore_signal(barrier, inc=1, device_id=dev, device_id_type=pl.DeviceIdType.MESH)
    pl.semaphore_wait(barrier, 8)

    sw_v = rc(wv, rows(WV, z * KR + y * 64, 64), s_sw.at[0], r_sw.at[0], partner)
    sw_k = rc(wk, rows(WK, z * KR + y * 64, 64), s_sw.at[1], r_sw.at[1], partner)
    sw_g = rc(GM.at[0], GM.at[1], s_sw.at[2], r_sw.at[2], partner)

    def tok(xx, j, half=None):
        cols = pl.ds(pl.multiple_of((xx * 4 + j) * 256, 256), 256)
        if half is None:
            return XB.at[1, :, :, cols]
        return XB.at[1, half, :, cols]

    def sw_t(j):
        cols = pl.ds(pl.multiple_of((x * 4 + j) * 256, 256), 256)
        return rc(prompt.at[:, :, cols], tok(x, j), s_sw.at[3 + j], r_sw.at[3 + j], partner)

    def t1(way, j, xx):
        return rc(tok(xx, j), tok(xx, j), s_tx.at[way, j], r_tx.at[way, j], (xp, xm)[way])

    def t2(way, j, xx):
        q = wrap(xx - 1, nx) if way == 0 else wrap(xx + 1, nx)
        return rc(tok(q, j, way), tok(q, j, way), s_tx.at[2 + way, j], r_tx.at[2 + way, j], (xp, xm)[way])

    @pl.when(swapped)
    def _():
        sw_v.start()
        sw_k.start()
        for j in range(4):
            sw_t(j).start()

    def zk(way, s, zz):
        b = wrap(zz - (s - 1), nz) if way == 0 else wrap(zz + (s - 1), nz)
        ref = rows(WK, b * KR + c * 128, 128) if s < 8 else rows(WK, b * KR + c * 128 + way * 64, 64)
        return rc(ref, ref, s_ag.at[way, s], r_ag.at[way, s], (zp, zm)[way])

    def zv(way, s, zz, who):
        b = wrap(zz - (s - 1), nz) if way == 0 else wrap(zz + (s - 1), nz)
        ref = rows(WV, b * KR + who * 64, 64) if s < 8 else rows(WV, b * KR + who * 64 + way * 32, 32)
        return rc(ref, ref, s_ag.at[2 + way, s], r_ag.at[2 + way, s], (zp, zm)[way])

    def blocks(s):
        if s == 0 or s == 8:
            return ((0, wrap(z - s, nz)),)
        return ((0, wrap(z - s, nz)), (1, wrap(z + s, nz)))

    def yv(s, who):
        out = []
        for k, b in blocks(s):
            ref = rows(WV, b * KR + who * 64, 64)
            out.append(rc(ref, ref, s_ag.at[4 + k, s], r_ag.at[4 + k, s], yp))
        return out

    def dk(s, cc):
        out = []
        for k, b in blocks(s):
            ref = rows(WK, b * KR + cc * 128, 128)
            out.append(rc(ref, ref, s_ag.at[6 + k, s], r_ag.at[6 + k, s], sib))
        return out

    def dv(s, cc):
        out = []
        for k, b in blocks(s):
            ref = rows(WV, b * KR + cc * 128, 128)
            out.append(rc(ref, ref, s_ag.at[8 + k, s], r_ag.at[8 + k, s], sib))
        return out

    def start(copies):
        for cp in copies:
            cp.start()

    def wait_recv(copies):
        for cp in copies:
            cp.wait_recv()

    yk_send = rc(own_k, own_k, s_yk.at[0], r_yk.at[0], yp)
    other_k = rows(WK, z * KR + yo * 64, 64)
    yk_recv = rc(other_k, other_k, s_yk.at[0], r_yk.at[0], yp)
    got_v = rc(own_v, own_v, s_sw.at[0], r_sw.at[0], partner)
    got_k = rc(own_k, own_k, s_sw.at[1], r_sw.at[1], partner)

    @pl.when(native)
    def _():
        l_wv.wait()

    @pl.when(swapped)
    def _():
        got_v.wait_recv()

    zv(0, 1, z, yr).start()
    zv(1, 1, z, yr).start()

    @pl.when(native)
    def _():
        l_wk.wait()

    @pl.when(swapped)
    def _():
        got_k.wait_recv()

    yk_send.start()
    start(yv(0, yr))
    yk_recv.wait_recv()
    zk(0, 1, z).start()
    zk(1, 1, z).start()
    start(dk(0, c))

    l_prompt.wait()
    l_wi.wait()
    l_wf.wait()
    tokens = XB[0].reshape(384, 4096)
    lane8 = lax.broadcasted_iota(jnp.int32, (384, 8), 1)

    def gate(w, b):
        g = lax.dot_general(tokens, w[...], (((1,), (1,)), ((), ())), preferred_element_type=F32)
        g = jnp.sum(jnp.where(lane8 == tp, g, 0.0), axis=1, keepdims=True) + b
        return jnp.broadcast_to(g, (384, 128))

    gi = gate(WI, ib[tp])
    lf = log_sigmoid(gate(WF, fb[tp]))
    after = (lax.broadcasted_iota(jnp.int32, (192, 192), 1)
             > lax.broadcasted_iota(jnp.int32, (192, 192), 0)).astype(F32)
    row8 = lax.broadcasted_iota(jnp.int32, (8, 128), 0)
    stats = jnp.zeros((8, 128), F32)
    qtile = jnp.zeros((8, 128), F32)
    for s in range(2):
        part = lf[s * 192:(s + 1) * 192]
        lw = jnp.dot(after, part, precision=lax.Precision.HIGHEST, preferred_element_type=F32)
        lw = lw + gi[s * 192:(s + 1) * 192]
        total = jnp.sum(part, axis=0, keepdims=True)
        top = jnp.max(lw, axis=0, keepdims=True)
        GM[0, s * 192:(s + 1) * 192, :] = jnp.exp(lw - top) * scale
        stats = jnp.where(row8 == 2 * s, total, jnp.where(row8 == 2 * s + 1, top, stats))
        qs = nq[s:s + 1, :].astype(F32)
        qtile = jnp.where(row8 == 2 * s, qs[:, :128], jnp.where(row8 == 2 * s + 1, qs[:, 128:], qtile))
    GM[0, 384:392, :] = stats
    GM[0, 392:400, :] = qtile

    @pl.when(swapped)
    def _():
        sw_g.start()

    AK[...] = jnp.zeros_like(AK)
    AV[...] = jnp.zeros_like(AV)
    VE[:, 512:640] = jnp.ones((384, 128), BF16)
    kk = lax.broadcasted_iota(jnp.int32, (256, 512), 0)
    rr = lax.broadcasted_iota(jnp.int32, (256, 512), 1)
    for s in range(2):
        target = ((kk >> 2) & 3) * 128 + (kk >> 4) * 8 + s * 4 + (kk & 3)
        PB[s] = (rr == target).astype(F32).astype(BF16)

    def st(k):
        return rc(GM.at[role, pl.ds(384, 8)], ST.at[yr], s_st.at[k], r_st.at[k], (sib, yp, diag)[k])

    def step(s):
        zk(0, s, z - 1).wait_recv()
        if s < 8:
            zk(0, s + 1, z).start()
        zk(1, s, z + 1).wait_recv()
        if s < 8:
            zk(1, s + 1, z).start()
        start(dk(s, c))
        zv(0, s, z - 1, yr).wait_recv()
        if s < 8:
            zv(0, s + 1, z, yr).start()
        zv(1, s, z + 1, yr).wait_recv()
        if s < 8:
            zv(1, s + 1, z, yr).start()
        start(yv(s, yr))
        wait_recv(yv(s - 1, yo))
        start(dv(s - 1, c))

    def token_step(s):
        if s <= 5:
            @pl.when(swapped)
            def _():
                if s <= 4:
                    j = s - 1
                    got = rc(tok(x, j), tok(x, j), s_sw.at[3 + j], r_sw.at[3 + j], partner)
                    got.wait_recv()
                    t1(0, j, x).start()
                    t1(1, j, x).start()
                if s >= 2:
                    j = s - 2
                    t1(0, j, wrap(x - 1, nx)).wait_recv()
                    t2(0, j, x).start()
                    t1(1, j, wrap(x + 1, nx)).wait_recv()
                    t2(1, j, x).start()

    for s in range(1, 4):
        step(s)
        token_step(s)

    @pl.when(swapped)
    def _():
        sw_g.wait_recv()

    ST[yr] = GM[role, 384:392, :]
    for k in range(3):
        st(k).start()
    step(4)
    token_step(4)
    step(5)
    token_step(5)
    for k in range(3):
        st(k).wait_recv()
    mz, tz = [], []
    for s in range(2):
        later = jnp.zeros((1, 128), F32)
        lifts = [None] * Y
        for k in reversed(range(Y)):
            lifts[k] = ST[k, 2 * s + 1:2 * s + 2, :] + later
            later = later + ST[k, 2 * s:2 * s + 1, :]
        top = jnp.maximum(jnp.maximum(lifts[0], lifts[1]), jnp.maximum(lifts[2], lifts[3]))
        mine = lifts[3]
        for k in range(3):
            mine = jnp.where(yr == k, lifts[k], mine)
        SC[s * 192:(s + 1) * 192, :] = GM[role, s * 192:(s + 1) * 192, :] * jnp.exp(mine - top)
        mz.append(top)
        tz.append(later)
    step(6)
    step(7)

    @pl.when(swapped)
    def _():
        for j in range(4):
            t2(0, j, wrap(x - 1, nx)).wait_recv()
            t2(1, j, wrap(x + 1, nx)).wait_recv()

    def mm(b):
        xc = XB[role, :, :, pl.ds(pl.multiple_of(b * KR, KR), KR)].reshape(384, KR)
        r = pl.ds(pl.multiple_of(b * KR, KR), KR)
        AK[...] += jnp.dot(xc, WK[r, :], preferred_element_type=F32)
        AV[...] += jnp.dot(xc, WV[r, :], preferred_element_type=F32)

    def wait_d(s):
        wait_recv(dk(s, 1 - c))
        wait_recv(dv(s, 1 - c))

    def mm_pair(s):
        def one(i, carry):
            mm(wrap(z + (2 * i - 1) * s, nz))
            return carry
        lax.fori_loop(0, 2, one, 0)

    for s in range(6):
        wait_d(s)

    def early(i, carry):
        mm(wrap(z + i - 5, nz))
        return carry

    lax.fori_loop(0, 11, early, 0)
    step(8)
    wait_d(6)
    mm_pair(6)
    wait_recv(yv(8, yo))
    start(dv(8, c))
    wait_d(7)
    mm_pair(7)
    wait_d(8)
    mm(wrap(z + 8, nz))

    for s in range(2):
        sc = SC[s * 192:(s + 1) * 192, :]
        kd = (AK[s * 192:(s + 1) * 192, :] * jnp.concatenate([sc, sc], axis=1)).astype(BF16)
        KC[s * 192:(s + 1) * 192, :] = jnp.dot(kd, PB[s], preferred_element_type=F32).astype(BF16)
    VE[:, 0:512] = AV[...].astype(BF16)

    def state(h):
        cols = pl.ds(pl.multiple_of(h * 256, 256), 256)
        out = lax.dot_general(KC[:, cols], VE[...], (((0,), (0,)), ((), ())), preferred_element_type=F32)
        SF[cols, :] = out
        SB[cols, :] = out.astype(BF16)

    ys1 = rc(rows(SB, (1 - c) * 256, 256), R1, s_ys.at[0], r_ys.at[0], sib)
    ys2 = rc(S2, R2, s_ys.at[1], r_ys.at[1], yp)
    state(1 - c)
    ys1.start()
    state(c)
    qsum = []
    sf_lo = (SF[...] - SB[...].astype(F32)).astype(BF16)
    for s in range(2):
        qs = jnp.concatenate([GM[role, 392 + 2 * s:393 + 2 * s, :], GM[role, 393 + 2 * s:394 + 2 * s, :]], axis=1)
        qs = jnp.broadcast_to(qs, (16, 256)).astype(BF16)
        qc = jnp.dot(qs, PB[s], preferred_element_type=F32).astype(BF16)
        full = jnp.dot(qc, SB[...], preferred_element_type=F32) + jnp.dot(qc, sf_lo, preferred_element_type=F32)
        qsum.append(full[0:8])
    row640 = lax.broadcasted_iota(jnp.int32, (8, 640), 0)
    both = jnp.where(row640 < 4, qsum[0], qsum[1])
    qt = jnp.zeros((8, 128), F32)
    for k in range(4):
        qt = qt + jnp.where((row8 & 3) == k, both[:, k * 128:(k + 1) * 128], 0.0)
    QM[0:8, :] = qt
    QM[8:16, :] = both[:, 512:640]

    def qm(k):
        return rc(QM, QR.at[k], s_qm.at[k], r_qm.at[k], (sib, yp, diag)[k])

    for k in range(3):
        qm(k).start()
    ys1.wait_recv()
    send_rows = pl.ds(pl.multiple_of(yo * 128, 128), 128)
    keep_rows = pl.ds(pl.multiple_of(yr * 128, 128), 128)
    send_part = pl.ds(pl.multiple_of((yo % 2) * 128, 128), 128)
    keep_part = pl.ds(pl.multiple_of((yr % 2) * 128, 128), 128)
    S2[...] = (SF[send_rows, :] + R1[send_part, :].astype(F32)).astype(BF16)
    ys2.start()
    kept = SF[keep_rows, :] + R1[keep_part, :].astype(F32)
    for k in range(3):
        qm(k).wait_recv()
    qall = QM[...] + QR[0] + QR[1] + QR[2]
    qt, qn = qall[0:8], qall[8:16]
    lane8 = lax.broadcasted_iota(jnp.int32, (8, 128), 1)
    head = jnp.zeros((8, 128), F32)
    m8 = jnp.where(row8 < 4, mz[0], mz[1])
    t8 = jnp.where(row8 < 4, tz[0], tz[1])
    for base, v in ((2, m8), (5, t8), (8, qn)):
        for i, piece in enumerate(three(v)):
            head = jnp.where(lane8 == base + i, piece, head)
    MB[:, :, 640:768] = jnp.broadcast_to(qt.astype(BF16)[None], (nz, 8, 128))
    ys2.wait_recv()
    kept = (kept + R2[...].astype(F32)).reshape(nz, 8, 640)
    MB[:, :, 0:512] = kept[:, :, 0:512].astype(BF16)
    norm = kept[:, :, 512:640]
    norm_hi = norm.astype(BF16).astype(F32)
    lane3 = lax.broadcasted_iota(jnp.int32, (nz, 8, 128), 2)
    tail = jnp.where(lane3 == 0, norm_hi, jnp.where(lane3 == 1, norm - norm_hi, head[None]))
    MB[:, :, 512:640] = tail.astype(BF16)

    oy = jnp.where(swapped, 3 - y, y)
    oc = jnp.where(swapped, 1 - c, c)

    def zs(to):
        return rc(MB.at[to], RB.at[z], s_zs.at[to], r_zs.at[z], at(x, oy, to, oc))

    def zs_recv(frm):
        return rc(MB.at[frm], RB.at[frm], s_zs.at[frm], r_zs.at[frm], at(x, oy, frm, oc))

    for d in (8, 7, -7, 6, -6, 5, -5, 4, -4, 3, -3, 2, -2, 1, -1):
        zs(wrap(z + d, nz)).start()

    @pl.when(swapped)
    def _():
        zs(z).start()

    @pl.when(native)
    def _():
        RB[z] = MB[z]

    for d in (1, -1, 2, -2, 3, -3, 4, -4, 5, -5, 6, -6, 7, -7, 8):
        zs_recv(wrap(z + d, nz)).wait_recv()

    @pl.when(swapped)
    def _():
        zs_recv(z).wait_recv()

    tails = RB[:, :, 512:640].astype(F32)
    m_all = jnp.sum(jnp.where((lane3 >= 2) & (lane3 < 5), tails, 0.0), axis=2, keepdims=True)
    t_all = jnp.sum(jnp.where((lane3 >= 5) & (lane3 < 8), tails, 0.0), axis=2, keepdims=True)
    later = jnp.zeros((8, 1), F32)
    lifts = [None] * nz
    for k in reversed(range(nz)):
        lifts[k] = m_all[k] + later
        later = later + t_all[k]
    top = lifts[0]
    for k in range(1, nz):
        top = jnp.maximum(top, lifts[k])
    acc = jnp.zeros((8, 768), F32)
    for k in range(nz):
        acc = acc + jnp.exp(lifts[k] - top) * RB[k].astype(F32)
    tail = acc[:, 512:640]
    norm = jnp.sum(jnp.where(lane8 < 2, tail, 0.0), axis=1, keepdims=True)
    qn = jnp.sum(jnp.where((lane8 >= 8) & (lane8 < 11), tail, 0.0), axis=1, keepdims=True)
    row1 = lax.broadcasted_iota(jnp.int32, (8, 1), 0)
    gate_in = jnp.where(row1 < 4, ng[0, :, 0:1], ng[0, :, 1:2])
    gate_forget = log_sigmoid(jnp.where(row1 < 4, ng[1, :, 0:1], ng[1, :, 1:2]))
    own = [jnp.sum(nq[s:s + 1, :].astype(F32) * nk[s:s + 1, :].astype(F32), axis=1, keepdims=True) * scale for s in range(2)]
    own = jnp.where(row1 < 4, own[0], own[1])
    mixed = jnp.maximum(gate_forget + top, gate_in)
    carried = jnp.exp(gate_forget + top - mixed)
    fresh = jnp.exp(gate_in - mixed)
    value = jnp.zeros((8, 128), F32)
    for s in range(2):
        for k in range(4):
            value = jnp.where(row8 == 4 * s + k, nv[s:s + 1, k * 128:(k + 1) * 128].astype(F32), value)
    numer = carried * acc[:, 640:768] + fresh * own * value
    denom = carried * qn + fresh * own
    read = numer / jnp.maximum(jnp.abs(denom), 1.0)
    out[:, 0:512] = acc[:, 0:512]
    out[:, 512:640] = jnp.where(lane8 == 0, top, norm)
    out[:, 640:768] = read

    for s in range(1, 9):
        for way in range(2):
            zk(way, s, z).wait_send()
            zv(way, s, z, yr).wait_send()
    for s in range(9):
        for cp in yv(s, yr) + dk(s, c) + dv(s, c):
            cp.wait_send()
    yk_send.wait_send()
    for k in range(3):
        st(k).wait_send()
        qm(k).wait_send()
    ys1.wait_send()
    ys2.wait_send()
    for d in range(1, 16):
        zs(wrap(z + d - 16, nz)).wait_send()

    @pl.when(swapped)
    def _():
        zs(z).wait_send()
        sw_v.wait_send()
        sw_k.wait_send()
        sw_g.wait_send()
        for j in range(4):
            sw_t(j).wait_send()
            for way in range(2):
                t1(way, j, x).wait_send()
                t2(way, j, x).wait_send()


def unpack(got, o_mem, o_norm, o_max, o_read):
    row = lax.broadcasted_iota(jnp.int32, (8, 128), 0)
    lane = lax.broadcasted_iota(jnp.int32, (8, 128), 1)
    tail = got[:, 512:640]
    top, norm = tail[:, 0:1], tail[:, 1:2]
    o_max[...] = jnp.sum(jnp.where(row == 4 * lane, top, 0.0), axis=0, keepdims=True)[:, 0:2]
    for s in range(2):
        o_mem[s, 0] = got[4 * s:4 * s + 4, 0:512].astype(BF16)
        line = jnp.sum(jnp.where(row - 4 * s == lane, norm, 0.0), axis=0, keepdims=True)
        o_norm[s] = line[:, 0:4]
        for k in range(4):
            at = 4 * s + k
            o_read[s:s + 1, k * 128:(k + 1) * 128] = got[at:at + 1, 640:768].astype(BF16)


def per_device(prompt, w_key, w_value, w_igate, w_fgate, input_bias, forget_bias, new_query, new_key, new_value,
               new_gates):
    nz = lax.axis_size("sp") // Y
    nx = lax.axis_size("tp") // 2
    vm = pl.BlockSpec(memory_space=pltpu.VMEM)
    sm = pl.BlockSpec(memory_space=pltpu.SMEM)
    hb = pl.BlockSpec(memory_space=pltpu.HBM)
    dma = pltpu.SemaphoreType.DMA
    packed = pl.pallas_call(
        lambda *refs: kernel(nz, nx, *refs),
        out_shape=jax.ShapeDtypeStruct((8, 768), F32),
        in_specs=[hb] * 5 + [sm] * 2 + [vm] * 4,
        out_specs=vm,
        scratch_shapes=[
            pltpu.VMEM((2, 2, 192, 4096), BF16),
            pltpu.VMEM((8, 4096), BF16),
            pltpu.VMEM((8, 4096), BF16),
            pltpu.VMEM((4096, 256), BF16),
            pltpu.VMEM((4096, 512), BF16),
            pltpu.VMEM((384, 256), F32),
            pltpu.VMEM((384, 512), F32),
            pltpu.VMEM((2, 400, 128), F32),
            pltpu.VMEM((4, 8, 128), F32),
            pltpu.VMEM((2, 256, 512), BF16),
            pltpu.VMEM((384, 512), BF16),
            pltpu.VMEM((384, 640), BF16),
            pltpu.VMEM((384, 128), F32),
            pltpu.VMEM((512, 640), F32),
            pltpu.VMEM((512, 640), BF16),
            pltpu.VMEM((256, 640), BF16),
            pltpu.VMEM((128, 640), BF16),
            pltpu.VMEM((128, 640), BF16),
            pltpu.VMEM((16, 128), F32),
            pltpu.VMEM((3, 16, 128), F32),
            pltpu.VMEM((nz, 8, 768), BF16),
            pltpu.VMEM((nz, 8, 768), BF16),
            dma((5,)),
            dma((10, 9)), dma((10, 9)),
            dma((1,)), dma((1,)),
            dma((7,)), dma((7,)),
            dma((4, 4)), dma((4, 4)),
            dma((3,)), dma((3,)),
            dma((3,)), dma((3,)),
            dma((2,)), dma((2,)),
            dma((nz,)), dma((nz,)),
        ],
        compiler_params=pltpu.CompilerParams(
            collective_id=0, has_side_effects=True, vmem_limit_bytes=56 * 1024 * 1024),
        name="prefill",
    )(
        prompt, w_key, w_value, w_igate.T, w_fgate.T, input_bias, forget_bias,
        new_query.reshape(2, 256), new_key.reshape(2, 256), new_value.reshape(2, 512),
        jnp.transpose(new_gates, (0, 2, 1)),
    )
    mem, norm, top, read = pl.pallas_call(
        unpack,
        out_shape=(
            jax.ShapeDtypeStruct((2, 1, 4, 512), BF16),
            jax.ShapeDtypeStruct((2, 1, 4), F32),
            jax.ShapeDtypeStruct((1, 2), F32),
            jax.ShapeDtypeStruct((2, 512), BF16),
        ),
        in_specs=[vm],
        out_specs=(vm,) * 4,
        name="unpack",
    )(packed)
    return mem, norm, top.T, read.reshape(2, 1, 512)


def solution(mesh):
    placed = (
        P(None, "sp", None),
        P("sp", "tp"),
        P("sp", "tp"),
        P(),
        P(),
        P(),
        P(),
        P(None, "tp", None),
        P(None, "tp", None),
        P(None, "tp", None),
        P(None, None, "tp"),
    )
    return jax.shard_map(
        per_device,
        mesh=mesh,
        in_specs=placed,
        out_specs=(
            P(None, "tp", "sp", None),
            P(None, "tp", "sp"),
            P(None, "tp"),
            P(None, "tp", None),
        ),
        check_vma=False,
    )
```

```python
import jax
import jax.numpy as jnp
from jax import lax
from jax.experimental import pallas as pl
from jax.experimental.pallas import tpu as pltpu
from jax.sharding import PartitionSpec as P

F32 = jnp.float32
BF16 = jnp.bfloat16
Y = 4
GROUP = (0, 0, 0, 1, 1, 2, 2, 3, 4)
KR = 256


def log_sigmoid(x):
    e = jnp.exp(-jnp.abs(x))
    series = e * (1.0 - e * (0.5 - e * (1.0 / 3.0 - e * (0.25 - e * 0.2))))
    return jnp.minimum(x, 0.0) - jnp.where(e < 0.04, series, jnp.log(1.0 + e))


def three(x):
    hi = x.astype(BF16).astype(F32)
    mid = (x - hi).astype(BF16).astype(F32)
    return hi, mid, x - hi - mid


def kernel(
    nz, nx,
    prompt, wk, wv, wi, wf, h_ib, h_fb, h_nq, h_nk, h_nv, h_ng,
    out,
    XB, WI, WF, WK, WV, AK, AV, GM, ST, PB, KC, VE, SC, SF, SB, R1, S2, R2, QM, QR, MA, MB, RA, RB,
    ib, fb, nq, nk, nv, ng,
    s_loc, s_k, s_v, s_y, s_d, r_z, r_y, r_d, s_yk, r_yk, s_sw, r_sw, s_t, r_t1, r_t2,
    s_st, r_st, s_qm, r_qm, s_ys, r_ys, s_zs, r_zs,
):
    sp = lax.axis_index("sp")
    tp = lax.axis_index("tp")
    z, y = sp // Y, sp % Y
    x, c = tp // 2, tp % 2
    parity = y // 2
    swapped = c != parity
    native = c == parity
    role = jnp.where(swapped, 1, 0)
    yr = jnp.where(swapped, 3 - y, y)
    yo = yr + 1 - 2 * (yr % 2)
    y1 = y + 1 - 2 * (y % 2)
    scale = 256 ** -0.5

    def at(x_, y_, z_, c_):
        return (z_ * Y + y_, x_ * 2 + c_)

    def wrap(v, n):
        return (v + n) % n

    zp, zm = at(x, y, wrap(z + 1, nz), c), at(x, y, wrap(z - 1, nz), c)
    xp, xm = at(wrap(x + 1, nx), y, z, c), at(wrap(x - 1, nx), y, z, c)
    sib, yp, diag = at(x, y, z, 1 - c), at(x, y1, z, c), at(x, y1, z, 1 - c)
    partner = at(x, 3 - y, z, 1 - c)

    def rc(src, dst, ss, rs, dev):
        return pltpu.make_async_remote_copy(
            src_ref=src, dst_ref=dst, send_sem=ss, recv_sem=rs, device_id=dev,
            device_id_type=pl.DeviceIdType.MESH)

    def rows(ref, start, n):
        return ref.at[pl.ds(pl.multiple_of(start, 32), n)]

    barrier = pltpu.get_barrier_semaphore()
    for dev in (zp, zm, xp, xm, sib, yp, diag, partner):
        pl.semaphore_signal(barrier, inc=1, device_id=dev, device_id_type=pl.DeviceIdType.MESH)

    l_prompt = pltpu.make_async_copy(prompt, XB.at[0], s_loc.at[0])
    l_wi = pltpu.make_async_copy(wi, WI, s_loc.at[1])
    l_wf = pltpu.make_async_copy(wf, WF, s_loc.at[2])
    own_k = rows(WK, z * KR + yr * 64, 64)
    own_v = rows(WV, z * KR + yr * 64, 64)
    l_wk = pltpu.make_async_copy(wk, own_k, s_loc.at[3])
    l_wv = pltpu.make_async_copy(wv, own_v, s_loc.at[4])

    @pl.when(native)
    def _():
        l_wv.start()
        l_wk.start()

    l_prompt.start()
    l_wi.start()
    l_wf.start()
    small = [pltpu.make_async_copy(a, b, s_loc.at[5 + i]) for i, (a, b) in enumerate(
        ((h_ib, ib), (h_fb, fb), (h_nq, nq), (h_nk, nk), (h_nv, nv), (h_ng, ng)))]
    for cp in small:
        cp.start()
    pl.semaphore_wait(barrier, 8)

    sw_v = rc(wv, rows(WV, z * KR + y * 64, 64), s_sw.at[0], r_sw.at[0], partner)
    sw_k = rc(wk, rows(WK, z * KR + y * 64, 64), s_sw.at[0], r_sw.at[1], partner)
    sw_g = rc(GM.at[0], GM.at[1], s_sw.at[1], r_sw.at[2], partner)

    def all_sent(ref, sem):
        rc(ref, ref, sem, sem, partner).wait_send()

    def all_here(ref, sem):
        rc(ref, ref, sem, sem, partner).wait_recv()

    def tok(xx, j, half=None):
        cols = pl.ds(pl.multiple_of((xx * 4 + j) * 256, 256), 256)
        if half is None:
            return XB.at[1, :, :, cols]
        return XB.at[1, half, :, cols]

    def sw_t(j):
        cols = pl.ds(pl.multiple_of((x * 4 + j) * 256, 256), 256)
        return rc(prompt.at[:, :, cols], tok(x, j), s_sw.at[2], r_sw.at[3 + j], partner)

    def t1(way, j, xx):
        return rc(tok(xx, j), tok(xx, j), s_t.at[0], r_t1.at[way, j], (xp, xm)[way])

    def t2(way, j, xx):
        q = wrap(xx - 1, nx) if way == 0 else wrap(xx + 1, nx)
        return rc(tok(q, j, way), tok(q, j, way), s_t.at[1], r_t2.at[0], (xp, xm)[way])

    @pl.when(swapped)
    def _():
        sw_v.start()
        sw_k.start()
        for j in range(4):
            sw_t(j).start()

    def zc(st, way, s, zz):
        b = wrap(zz - (s - 1), nz) if way == 0 else wrap(zz + (s - 1), nz)
        if st < 2:
            ref = rows(WK, b * KR + (yr, yo)[st] * 64, 64)
        else:
            ref = rows(WV, b * KR + yr * 64 + (st - 2) * 32, 32)
        slot = st * 15 + (14 if s == 8 else way * 7 + s - 1)
        return rc(ref, ref, (s_k if st < 2 else s_v).at[0], r_z.at[slot], (zp, zm)[way])

    def ways(st, s):
        return (0, 1) if s < 8 else (st % 2,)

    def blocks(s):
        if s == 0 or s == 8:
            return ((0, wrap(z - s, nz)),)
        return ((0, wrap(z - s, nz)), (1, wrap(z + s, nz)))

    def yv(s, who):
        out = []
        for k, b in blocks(s):
            ref = rows(WV, b * KR + who * 64, 64)
            out.append(rc(ref, ref, s_y.at[0], r_y.at[s], yp))
        return out

    def dk(s, cc):
        out = []
        for k, b in blocks(s):
            ref = rows(WK, b * KR + cc * 128, 128)
            out.append(rc(ref, ref, s_d.at[0], r_d.at[GROUP[s]], sib))
        return out

    def dv(s, cc):
        out = []
        for k, b in blocks(s):
            ref = rows(WV, b * KR + cc * 128, 128)
            out.append(rc(ref, ref, s_d.at[0], r_d.at[GROUP[s]], sib))
        return out

    def start(copies):
        for cp in copies:
            cp.start()

    def y_here(s):
        all_here(rows(WV, 0, 64 * len(blocks(s))), r_y.at[s])

    def d_here(g):
        n = sum(len(blocks(s)) for s in range(9) if GROUP[s] == g)
        all_here(rows(WV, 0, 192 * n), r_d.at[g])

    yk_send = rc(own_k, own_k, s_yk.at[0], r_yk.at[0], yp)
    other_k = rows(WK, z * KR + yo * 64, 64)
    yk_recv = rc(other_k, other_k, s_yk.at[0], r_yk.at[0], yp)
    got_v = rc(own_v, own_v, s_sw.at[0], r_sw.at[0], partner)
    got_k = rc(own_k, own_k, s_sw.at[1], r_sw.at[1], partner)

    @pl.when(native)
    def _():
        l_wv.wait()

    @pl.when(swapped)
    def _():
        got_v.wait_recv()

    for st in (2, 3):
        for way in (0, 1):
            zc(st, way, 1, z).start()
    start(yv(0, yr))

    @pl.when(native)
    def _():
        l_wk.wait()

    @pl.when(swapped)
    def _():
        got_k.wait_recv()

    yk_send.start()
    for way in (0, 1):
        zc(0, way, 1, z).start()
    l_prompt.wait()
    l_wi.wait()
    l_wf.wait()
    for cp in small:
        cp.wait()
    tokens = XB[0].reshape(384, 4096)
    lane8 = lax.broadcasted_iota(jnp.int32, (384, 8), 1)

    def gate(w, b):
        g = lax.dot_general(tokens, w[...], (((1,), (1,)), ((), ())), preferred_element_type=F32)
        g = jnp.sum(jnp.where(lane8 == tp, g + b[...], 0.0), axis=1, keepdims=True)
        return jnp.broadcast_to(g, (384, 128))

    gi = gate(WI, ib)
    lf = log_sigmoid(gate(WF, fb))
    after = (lax.broadcasted_iota(jnp.int32, (192, 192), 1)
             > lax.broadcasted_iota(jnp.int32, (192, 192), 0)).astype(F32)
    row8 = lax.broadcasted_iota(jnp.int32, (8, 128), 0)
    stats = jnp.zeros((8, 128), F32)
    qtile = jnp.zeros((8, 128), F32)
    for s in range(2):
        part = lf[s * 192:(s + 1) * 192]
        lw = jnp.dot(after, part, precision=lax.Precision.HIGHEST, preferred_element_type=F32)
        lw = lw + gi[s * 192:(s + 1) * 192]
        total = jnp.sum(part, axis=0, keepdims=True)
        top = jnp.max(lw, axis=0, keepdims=True)
        GM[0, s * 192:(s + 1) * 192, :] = jnp.exp(lw - top) * scale
        stats = jnp.where(row8 == 2 * s, total, jnp.where(row8 == 2 * s + 1, top, stats))
        qs = nq[s:s + 1, :].astype(F32)
        qtile = jnp.where(row8 == 2 * s, qs[:, :128], jnp.where(row8 == 2 * s + 1, qs[:, 128:], qtile))
    GM[0, 384:392, :] = stats
    GM[0, 392:400, :] = qtile

    @pl.when(swapped)
    def _():
        sw_g.start()

    yk_recv.wait_recv()
    for way in (0, 1):
        zc(1, way, 1, z).start()
    start(dk(0, c))

    AK[...] = jnp.zeros_like(AK)
    AV[...] = jnp.zeros_like(AV)
    VE[:, 512:640] = jnp.ones((384, 128), BF16)
    kk = lax.broadcasted_iota(jnp.int32, (256, 512), 0)
    rr = lax.broadcasted_iota(jnp.int32, (256, 512), 1)
    for s in range(2):
        target = ((kk >> 2) & 3) * 128 + (kk >> 4) * 8 + s * 4 + (kk & 3)
        PB[s] = (rr == target).astype(F32).astype(BF16)

    def st(k):
        return rc(GM.at[role, pl.ds(384, 8)], ST.at[yr], s_st.at[0], r_st.at[0], (sib, yp, diag)[k])

    def step(s):
        for st in (2, 3, 0, 1):
            for way in ways(st, s):
                zc(st, way, s, (z - 1, z + 1)[way]).wait_recv()
                if s < 8 and way in ways(st, s + 1):
                    zc(st, way, s + 1, z).start()
            if st == 3:
                start(yv(s, yr))
        start(dk(s, c))
        if s >= 2:
            pass_on(s - 2)

    def pass_on(s):
        y_here(s)
        start(dv(s, c))

    def token_step(s):
        if s <= 5:
            @pl.when(swapped)
            def _():
                if s <= 4:
                    j = s - 1
                    got = rc(tok(x, j), tok(x, j), s_sw.at[2], r_sw.at[3 + j], partner)
                    got.wait_recv()
                    t1(0, j, x).start()
                    t1(1, j, x).start()
                if s >= 2:
                    j = s - 2
                    t1(0, j, wrap(x - 1, nx)).wait_recv()
                    t2(0, j, x).start()
                    t1(1, j, wrap(x + 1, nx)).wait_recv()
                    t2(1, j, x).start()

    for s in range(1, 4):
        step(s)
        token_step(s)

    @pl.when(swapped)
    def _():
        sw_g.wait_recv()

    ST[yr] = GM[role, 384:392, :]
    for k in range(3):
        st(k).start()
    step(4)
    token_step(4)
    step(5)
    token_step(5)
    all_here(GM.at[0, pl.ds(0, 24)], r_st.at[0])
    mz, tz = [], []
    for s in range(2):
        later = jnp.zeros((1, 128), F32)
        lifts = [None] * Y
        for k in reversed(range(Y)):
            lifts[k] = ST[k, 2 * s + 1:2 * s + 2, :] + later
            later = later + ST[k, 2 * s:2 * s + 1, :]
        top = jnp.maximum(jnp.maximum(lifts[0], lifts[1]), jnp.maximum(lifts[2], lifts[3]))
        mine = lifts[3]
        for k in range(3):
            mine = jnp.where(yr == k, lifts[k], mine)
        SC[s * 192:(s + 1) * 192, :] = GM[role, s * 192:(s + 1) * 192, :] * jnp.exp(mine - top)
        mz.append(top)
        tz.append(later)
    step(6)
    def mm(b):
        xc = XB[role, :, :, pl.ds(pl.multiple_of(b * KR, KR), KR)].reshape(384, KR)
        r = pl.ds(pl.multiple_of(b * KR, KR), KR)
        AK[...] += jnp.dot(xc, WK[r, :], preferred_element_type=F32)
        AV[...] += jnp.dot(xc, WV[r, :], preferred_element_type=F32)

    def mm_pair(s):
        def one(i, carry):
            mm(wrap(z + (2 * i - 1) * s, nz))
            return carry
        lax.fori_loop(0, 2, one, 0)

    def early(i, carry):
        mm(wrap(z + i - 2, nz))
        return carry

    @pl.when(swapped)
    def _():
        all_here(XB.at[1, :, :, pl.ds(0, 1024)], r_t2.at[0])

    d_here(0)
    lax.fori_loop(0, 5, early, 0)
    step(7)
    d_here(1)
    mm_pair(3)
    mm_pair(4)
    step(8)
    pass_on(7)
    d_here(2)
    mm_pair(5)
    mm_pair(6)
    pass_on(8)
    d_here(3)
    mm_pair(7)
    d_here(4)
    mm(wrap(z + 8, nz))

    for s in range(2):
        sc = SC[s * 192:(s + 1) * 192, :]
        kd = (AK[s * 192:(s + 1) * 192, :] * jnp.concatenate([sc, sc], axis=1)).astype(BF16)
        KC[s * 192:(s + 1) * 192, :] = jnp.dot(kd, PB[s], preferred_element_type=F32).astype(BF16)
    VE[:, 0:512] = AV[...].astype(BF16)

    CUTS = (slice(0, 256), slice(256, 640))

    def state(h, i):
        half = pl.ds(pl.multiple_of(h * 256, 256), 256)
        part = lax.dot_general(KC[:, half], VE[:, CUTS[i]], (((0,), (0,)), ((), ())), preferred_element_type=F32)
        SF[half, CUTS[i]] = part
        SB[half, CUTS[i]] = part.astype(BF16)

    def ys1(i):
        half = pl.ds(pl.multiple_of((1 - c) * 256, 256), 256)
        w = pl.ds(CUTS[i].start, CUTS[i].stop - CUTS[i].start)
        return rc(SB.at[half, w], R1.at[:, w], s_ys.at[0], r_ys.at[i], sib)

    def ys2(i):
        w = pl.ds(CUTS[i].start, CUTS[i].stop - CUTS[i].start)
        return rc(S2.at[:, w], R2.at[:, w], s_ys.at[0], r_ys.at[2 + i], yp)

    send_rows = pl.ds(pl.multiple_of(yo * 128, 128), 128)
    keep_rows = pl.ds(pl.multiple_of(yr * 128, 128), 128)
    send_part = pl.ds(pl.multiple_of((yo % 2) * 128, 128), 128)
    keep_part = pl.ds(pl.multiple_of((yr % 2) * 128, 128), 128)

    def pair_sum(i):
        ys1(i).wait_recv()
        S2[:, CUTS[i]] = (SF[send_rows, CUTS[i]] + R1[send_part, CUTS[i]].astype(F32)).astype(BF16)
        ys2(i).start()

    def kept(i):
        ys2(i).wait_recv()
        part = SF[keep_rows, CUTS[i]] + R1[keep_part, CUTS[i]].astype(F32) + R2[:, CUTS[i]].astype(F32)
        return part.reshape(nz, 8, CUTS[i].stop - CUTS[i].start)

    oy = jnp.where(swapped, 3 - y, y)
    oc = jnp.where(swapped, 1 - c, c)

    def zs(i, to):
        return rc((MA, MB)[i].at[to], (RA, RB)[i].at[z], s_zs.at[i], r_zs.at[i], at(x, oy, to, oc))

    def zsend(i):
        for d in (8, 7, -7, 6, -6, 5, -5, 4, -4, 3, -3, 2, -2, 1, -1):
            zs(i, wrap(z + d, nz)).start()

        @pl.when(swapped)
        def _():
            zs(i, z).start()

        @pl.when(native)
        def _():
            (RA, RB)[i][z] = (MA, MB)[i][z]

    state(1 - c, 0)
    ys1(0).start()
    state(c, 0)
    state(1 - c, 1)
    ys1(1).start()
    state(c, 1)
    pair_sum(0)
    qsum = []
    sf_lo = (SF[...] - SB[...].astype(F32)).astype(BF16)
    for s in range(2):
        qs = jnp.concatenate([GM[role, 392 + 2 * s:393 + 2 * s, :], GM[role, 393 + 2 * s:394 + 2 * s, :]], axis=1)
        qs = jnp.broadcast_to(qs, (16, 256)).astype(BF16)
        qc = jnp.dot(qs, PB[s], preferred_element_type=F32).astype(BF16)
        full = jnp.dot(qc, SB[...], preferred_element_type=F32) + jnp.dot(qc, sf_lo, preferred_element_type=F32)
        qsum.append(full[0:8])
    row640 = lax.broadcasted_iota(jnp.int32, (8, 640), 0)
    both = jnp.where(row640 < 4, qsum[0], qsum[1])
    qt = jnp.zeros((8, 128), F32)
    for k in range(4):
        qt = qt + jnp.where((row8 & 3) == k, both[:, k * 128:(k + 1) * 128], 0.0)
    QM[0:8, :] = qt
    QM[8:16, :] = both[:, 512:640]

    def qm(k):
        return rc(QM, QR.at[k], s_qm.at[0], r_qm.at[0], (sib, yp, diag)[k])

    for k in range(3):
        qm(k).start()
    pair_sum(1)
    MA[...] = kept(0).astype(BF16)
    zsend(0)
    all_here(GM.at[0, pl.ds(0, 48)], r_qm.at[0])
    qall = QM[...] + QR[0] + QR[1] + QR[2]
    qt, qn = qall[0:8], qall[8:16]
    lane8 = lax.broadcasted_iota(jnp.int32, (8, 128), 1)
    head = jnp.zeros((8, 128), F32)
    m8 = jnp.where(row8 < 4, mz[0], mz[1])
    t8 = jnp.where(row8 < 4, tz[0], tz[1])
    for base, v in ((2, m8), (5, t8), (8, qn)):
        for i, piece in enumerate(three(v)):
            head = jnp.where(lane8 == base + i, piece, head)
    MB[:, :, 384:512] = jnp.broadcast_to(qt.astype(BF16)[None], (nz, 8, 128))
    part = kept(1)
    MB[:, :, 0:256] = part[:, :, 0:256].astype(BF16)
    norm = part[:, :, 256:384]
    norm_hi = norm.astype(BF16).astype(F32)
    lane3 = lax.broadcasted_iota(jnp.int32, (nz, 8, 128), 2)
    tail = jnp.where(lane3 == 0, norm_hi, jnp.where(lane3 == 1, norm - norm_hi, head[None]))
    MB[:, :, 256:384] = tail.astype(BF16)
    zsend(1)

    for i in range(2):
        @pl.when(native)
        def _():
            all_here((RA, RB)[i].at[pl.ds(0, nz - 1)], r_zs.at[i])

        @pl.when(swapped)
        def _():
            all_here((RA, RB)[i], r_zs.at[i])

    tails = RB[:, :, 256:384].astype(F32)
    m_all = jnp.sum(jnp.where((lane3 >= 2) & (lane3 < 5), tails, 0.0), axis=2, keepdims=True)
    t_all = jnp.sum(jnp.where((lane3 >= 5) & (lane3 < 8), tails, 0.0), axis=2, keepdims=True)
    later = jnp.zeros((8, 1), F32)
    lifts = [None] * nz
    for k in reversed(range(nz)):
        lifts[k] = m_all[k] + later
        later = later + t_all[k]
    top = lifts[0]
    for k in range(1, nz):
        top = jnp.maximum(top, lifts[k])
    first = jnp.zeros((8, 256), F32)
    acc = jnp.zeros((8, 512), F32)
    for k in range(nz):
        weight = jnp.exp(lifts[k] - top)
        first = first + weight * RA[k].astype(F32)
        acc = acc + weight * RB[k].astype(F32)
    tail = acc[:, 256:384]
    norm = jnp.sum(jnp.where(lane8 < 2, tail, 0.0), axis=1, keepdims=True)
    qn = jnp.sum(jnp.where((lane8 >= 8) & (lane8 < 11), tail, 0.0), axis=1, keepdims=True)
    row1 = lax.broadcasted_iota(jnp.int32, (8, 1), 0)
    gate_in = jnp.where(row1 < 4, ng[0, :, 0:1], ng[0, :, 1:2])
    gate_forget = log_sigmoid(jnp.where(row1 < 4, ng[1, :, 0:1], ng[1, :, 1:2]))
    own = [jnp.sum(nq[s:s + 1, :].astype(F32) * nk[s:s + 1, :].astype(F32), axis=1, keepdims=True) * scale for s in range(2)]
    own = jnp.where(row1 < 4, own[0], own[1])
    mixed = jnp.maximum(gate_forget + top, gate_in)
    carried = jnp.exp(gate_forget + top - mixed)
    fresh = jnp.exp(gate_in - mixed)
    value = jnp.zeros((8, 128), F32)
    for s in range(2):
        for k in range(4):
            value = jnp.where(row8 == 4 * s + k, nv[s:s + 1, k * 128:(k + 1) * 128].astype(F32), value)
    numer = carried * acc[:, 384:512] + fresh * own * value
    denom = carried * qn + fresh * own
    read = numer / jnp.maximum(jnp.abs(denom), 1.0)
    out[:, 0:256] = first
    out[:, 256:512] = acc[:, 0:256]
    out[:, 512:640] = jnp.where(lane8 == 0, top, norm)
    out[:, 640:768] = read

    all_sent(rows(WK, 0, 1920), s_k.at[0])
    all_sent(rows(WV, 0, 960), s_v.at[0])
    all_sent(rows(WV, 0, 1024), s_y.at[0])
    all_sent(rows(WV, 0, 3072), s_d.at[0])
    yk_send.wait_send()
    all_sent(GM.at[0, pl.ds(0, 24)], s_st.at[0])
    all_sent(GM.at[0, pl.ds(0, 48)], s_qm.at[0])
    all_sent(rows(SB, 0, 384), s_ys.at[0])
    for i in range(2):
        @pl.when(native)
        def _():
            all_sent((MA, MB)[i].at[pl.ds(0, nz - 1)], s_zs.at[i])

        @pl.when(swapped)
        def _():
            all_sent((MA, MB)[i], s_zs.at[i])

    @pl.when(swapped)
    def _():
        all_sent(rows(WV, 0, 96), s_sw.at[0])
        sw_g.wait_send()
        all_sent(XB.at[1, :, :, pl.ds(0, 1024)], s_sw.at[2])
        all_sent(XB.at[1, :, :, pl.ds(0, 2048)], s_t.at[0])
        all_sent(XB.at[1, :, :, pl.ds(0, 1024)], s_t.at[1])


def unpack(got, o_mem, o_norm, o_max, o_read):
    row = lax.broadcasted_iota(jnp.int32, (8, 128), 0)
    lane = lax.broadcasted_iota(jnp.int32, (8, 128), 1)
    tail = got[:, 512:640]
    top, norm = tail[:, 0:1], tail[:, 1:2]
    o_max[...] = jnp.sum(jnp.where(row == 4 * lane, top, 0.0), axis=0, keepdims=True)[:, 0:2]
    for s in range(2):
        o_mem[s, 0] = got[4 * s:4 * s + 4, 0:512].astype(BF16)
        line = jnp.sum(jnp.where(row - 4 * s == lane, norm, 0.0), axis=0, keepdims=True)
        o_norm[s] = line[:, 0:4]
        for k in range(4):
            at = 4 * s + k
            o_read[s:s + 1, k * 128:(k + 1) * 128] = got[at:at + 1, 640:768].astype(BF16)


def per_device(prompt, w_key, w_value, w_igate, w_fgate, input_bias, forget_bias, new_query, new_key, new_value,
               new_gates):
    nz = lax.axis_size("sp") // Y
    nx = lax.axis_size("tp") // 2
    vm = pl.BlockSpec(memory_space=pltpu.VMEM)
    hb = pl.BlockSpec(memory_space=pltpu.HBM)
    dma = pltpu.SemaphoreType.DMA
    packed = pl.pallas_call(
        lambda *refs: kernel(nz, nx, *refs),
        out_shape=jax.ShapeDtypeStruct((8, 768), F32),
        in_specs=[hb] * 11,
        out_specs=vm,
        scratch_shapes=[
            pltpu.VMEM((2, 2, 192, 4096), BF16),
            pltpu.VMEM((8, 4096), BF16),
            pltpu.VMEM((8, 4096), BF16),
            pltpu.VMEM((4096, 256), BF16),
            pltpu.VMEM((4096, 512), BF16),
            pltpu.VMEM((384, 256), F32),
            pltpu.VMEM((384, 512), F32),
            pltpu.VMEM((2, 400, 128), F32),
            pltpu.VMEM((4, 8, 128), F32),
            pltpu.VMEM((2, 256, 512), BF16),
            pltpu.VMEM((384, 512), BF16),
            pltpu.VMEM((384, 640), BF16),
            pltpu.VMEM((384, 128), F32),
            pltpu.VMEM((512, 640), F32),
            pltpu.VMEM((512, 640), BF16),
            pltpu.VMEM((256, 640), BF16),
            pltpu.VMEM((128, 640), BF16),
            pltpu.VMEM((128, 640), BF16),
            pltpu.VMEM((16, 128), F32),
            pltpu.VMEM((3, 16, 128), F32),
            pltpu.VMEM((nz, 8, 256), BF16),
            pltpu.VMEM((nz, 8, 512), BF16),
            pltpu.VMEM((nz, 8, 256), BF16),
            pltpu.VMEM((nz, 8, 512), BF16),
            pltpu.VMEM((1, 8), F32),
            pltpu.VMEM((1, 8), F32),
            pltpu.VMEM((2, 256), BF16),
            pltpu.VMEM((2, 256), BF16),
            pltpu.VMEM((2, 512), BF16),
            pltpu.VMEM((2, 1, 2), F32),
            dma((11,)), dma((1,)), dma((1,)), dma((1,)), dma((1,)), dma((60,)), dma((9,)), dma((5,)),
            dma((1,)), dma((1,)), dma((3,)), dma((7,)), dma((2,)), dma((2, 4)), dma((1,)),
            dma((1,)), dma((1,)), dma((1,)), dma((1,)), dma((1,)), dma((4,)), dma((2,)), dma((2,)),
        ],
        compiler_params=pltpu.CompilerParams(
            collective_id=0, has_side_effects=True, vmem_limit_bytes=56 * 1024 * 1024),
        name="prefill",
    )(
        prompt, w_key, w_value, w_igate.T, w_fgate.T, input_bias.reshape(1, 8), forget_bias.reshape(1, 8),
        new_query.reshape(2, 256), new_key.reshape(2, 256), new_value.reshape(2, 512),
        jnp.transpose(new_gates, (0, 2, 1)),
    )
    mem, norm, top, read = pl.pallas_call(
        unpack,
        out_shape=(
            jax.ShapeDtypeStruct((2, 1, 4, 512), BF16),
            jax.ShapeDtypeStruct((2, 1, 4), F32),
            jax.ShapeDtypeStruct((1, 2), F32),
            jax.ShapeDtypeStruct((2, 512), BF16),
        ),
        in_specs=[vm],
        out_specs=(vm,) * 4,
        name="unpack",
    )(packed)
    return mem, norm, top.T, read.reshape(2, 1, 512)


def solution(mesh):
    placed = (
        P(None, "sp", None),
        P("sp", "tp"),
        P("sp", "tp"),
        P(),
        P(),
        P(),
        P(),
        P(None, "tp", None),
        P(None, "tp", None),
        P(None, "tp", None),
        P(None, None, "tp"),
    )
    return jax.shard_map(
        per_device,
        mesh=mesh,
        in_specs=placed,
        out_specs=(
            P(None, "tp", "sp", None),
            P(None, "tp", "sp"),
            P(None, "tp"),
            P(None, "tp", None),
        ),
        check_vma=False,
    )
```
